32 devices in a mesh: grp: 2 (over y), fs: 4 (over z), tp: 4 (over x, core).
Axes of the slice: x: 2, y: 2, z: 4, core: 2. Of those that a mesh axis runs over, the one named last changes fastest.
Arguments:
- tokens: bfloat16 [4096, 2048], P(('grp', 'fs', 'tp')), parts along dimension 0, may hold values from -6 to 6
- route_ids: int32 [4096, 8], P(('grp', 'fs', 'tp')), parts along dimension 0, may hold values from 0 to 15, all different within a row; in each aligned block of 128 rows (0 to 127, 128 to 255, ...) at most 96 rows name the same one
- route_scores: float32 [4096, 8], P(('grp', 'fs', 'tp')), parts along dimension 0, may hold values from 0.05 to 1
- norm_gain: float32 [2048], P('fs'), may hold values from 0.1 to 1.9
- expert_gate: float32 [16, 2048, 256], P(None, 'fs', 'tp'), may hold values from -0.125 to 0.125
- expert_up: float32 [16, 2048, 256], P(None, 'fs', 'tp'), may hold values from -0.125 to 0.125
- expert_down: float32 [16, 256, 2048], P(None, 'fs', 'tp'), may hold values from -0.375 to 0.375
- shared_gate: float32 [2048, 256], P('fs', 'tp'), may hold values from -0.125 to 0.125
- shared_up: float32 [2048, 256], P('fs', 'tp'), may hold values from -0.125 to 0.125
- shared_down: float32 [256, 2048], P('fs', 'tp'), may hold values from -0.375 to 0.375
Outputs:
- mixed: bfloat16 [4096, 2048], P(('grp', 'fs', 'tp')), parts along dimension 0
- sampler_gate: bfloat16 [32, 2048, 256], P(('grp', 'fs', 'tp')), parts along dimension 0
- sampler_up: bfloat16 [32, 2048, 256], P(('grp', 'fs', 'tp')), parts along dimension 0
- sampler_down: bfloat16 [32, 256, 2048], P(('grp', 'fs', 'tp')), parts along dimension 0
- sampler_shared_gate: bfloat16 [4096, 256], P(('grp', 'fs')), parts along dimension 0
- sampler_shared_up: bfloat16 [4096, 256], P(('grp', 'fs')), parts along dimension 0
- sampler_shared_down: bfloat16 [512, 2048], P(('grp', 'fs')), parts along dimension 0
The draws below stay inside these ranges and needn't reach their ends.
There are 2 independent parts, one for each index of `grp`. The reference program is written for one: setup_inputs(seed, part) draws one part's arguments, and reference() takes and returns one part's arrays. A program takes and returns all parts, laid end to end along the dimension named above; an argument that names none is the same for every part. Nothing has to cross between parts.
Inputs may be any that keep to these rules, and one draw needn't show every extreme that they name: `route_ids`: each row names 8 different experts. Among the 128 rows of one device no expert is named more than 96 times, a bound that some block reaches.
All inputs are finite; a program needn't handle non-finite values.
Results may differ from the reference program's by a relative error of at most 0.0084.
Values may be sent and summed in bfloat16 or wider, within the bound.
A program may use at most 128 MiB of HBM per device.

```python
import math
import jax
import jax.numpy as jnp
import numpy as np
from jax import lax

D = 2048
F = 256
SH = 256
TOP_K = 8
TOK_DEV = 128
EXPERTS = 16
TOKENS = 2048
CAP = 96


def level_of(rng, extent, pieces, least, largest):
    def one(dim, blocks):
        draws = jax.random.uniform(jax.random.fold_in(jax.random.fold_in(rng, 6), dim), (blocks,), jnp.float32, least / len(pieces), largest / len(pieces))
        return jnp.repeat(jnp.exp(draws), extent[dim] // blocks).reshape((-1,) + (1,) * (len(extent) - dim - 1))

    factor_of = one(*pieces[0])
    for cut in pieces[1:]:
        factor_of = factor_of * one(*cut)
    return factor_of


def routed_block(own_key, own, number, rows, number_of, top, most, skew):
    ranking = jax.random.permutation(own_key, number_of)
    packed, usual = shares(number_of, rows * top, most, skew, True), shares(number_of, rows * top, most, skew, False)
    places = jnp.arange(number_of)

    def named(tallies, rotation):
        used = int((tallies > 0).sum())
        fixed = max(1, used // 4)
        moved = fixed + (places - fixed + rotation * (used - fixed)) % max(1, number_of - fixed)
        return jnp.zeros((number_of,), jnp.int32).at[ranking[jnp.where(places < fixed, places, moved)]].set(jnp.asarray(tallies, jnp.int32))

    tallies = jnp.where(number % 4 == 0, named(packed, number // 4), named(usual, number - number // 4 - 1))
    mixed = jax.random.permutation(jax.random.fold_in(own, 3), number_of)
    giver, taker = mixed[0:number_of // 2 * 2:2], mixed[1:number_of // 2 * 2:2]
    slack = jnp.minimum(tallies[giver] - 1, most - tallies[taker]) // 2
    slack = jnp.where((giver == ranking[0]) | (taker == ranking[0]) | (tallies[taker] == 0), 0, jnp.maximum(slack, 0))
    moved = jax.random.randint(jax.random.fold_in(own, 4), (number_of // 2,), 0, 1 << 20) % (slack + 1)
    tallies = tallies.at[giver].add(-moved).at[taker].add(moved)
    items = jnp.searchsorted(jnp.cumsum(tallies), jnp.arange(rows * top), side="right").astype(jnp.int32)
    listing = items.reshape(top, rows).T
    listing = listing[jax.random.permutation(jax.random.fold_in(own, 1), rows)]
    rotation = jax.random.randint(jax.random.fold_in(own, 2), (rows, 1), 0, top)
    return jnp.take_along_axis(listing, (jnp.arange(top)[None, :] + rotation) % top, axis=1)


def shares(amount, total, most, slope, full):
    weights = [(1 << 20) // math.isqrt(grade ** slope) + 1 for grade in range(1, amount + 1)]
    largest = most if full else min(most, max(-(-total // amount), total * weights[0] // sum(weights)))
    least = 1 if total - largest >= amount - 1 else 0
    given, surplus = [largest] + [least] * (amount - 1), total - largest - least * (amount - 1)
    while surplus > 0:
        movable = [i for i in range(1, amount) if given[i] < largest] or [i for i in range(1, amount) if given[i] < most]
        whole, left = sum([weights[i] for i in movable]), surplus
        for i in movable:
            addition = min(most - given[i], max(1, left * weights[i] // whole), surplus)
            given[i] = given[i] + addition
            surplus = surplus - addition
    return np.array(given)


def bell_draw(stream_key, shape, width, bound, pieces=(), held_as=jnp.bfloat16):
    result = jax.random.normal(stream_key, shape, jnp.float32) * width
    if len(pieces) > 0:
        result = level_of(stream_key, shape, pieces, -0.22, 0.18) * result
    return jnp.clip(result, min=-bound, max=bound).astype(held_as)


def setup_inputs(seed: int = 0, part: int = 0) -> dict:
    arg_keys = jax.random.split(jax.random.key(seed), 11)
    part_keys = jax.random.split(jax.random.fold_in(arg_keys[10], part), 11)
    tokens = bell_draw(part_keys[0], (TOKENS, D), 1.0, 6.0, ((0, 16),))
    route_ids_keys = jax.random.split(jax.random.fold_in(part_keys[1], 1), TOKENS // TOK_DEV)
    route_ids_turns = jax.random.permutation(jax.random.fold_in(part_keys[1], 3), TOKENS // TOK_DEV)
    route_ids = jax.vmap(lambda own, number: routed_block(jax.random.fold_in(part_keys[1], 2), own, number, TOK_DEV, EXPERTS, TOP_K, CAP, 1))(route_ids_keys, route_ids_turns).reshape((TOKENS, TOP_K))
    route_scores = jnp.clip(0.05 + 0.95 * jax.random.uniform(part_keys[2], (TOKENS, TOP_K), jnp.float32) ** level_of(part_keys[2], (TOKENS, TOP_K), ((0, 16),), -0.2, 0.2), 0.05, 1.0)
    norm_gain = jnp.clip(1.0 + 0.18 * jax.random.normal(arg_keys[3], (D,), jnp.float32), 0.1, 1.9)
    expert_gate = bell_draw(arg_keys[4], (EXPERTS, D, F), D ** -0.5, 0.125, ((1, 4), (2, 4)), jnp.float32)
    expert_up = bell_draw(arg_keys[5], (EXPERTS, D, F), D ** -0.5, 0.125, ((1, 4), (2, 4)), jnp.float32)
    expert_down = bell_draw(arg_keys[6], (EXPERTS, F, D), F ** -0.5, 0.375, ((1, 4), (2, 4)), jnp.float32)
    shared_gate = bell_draw(arg_keys[7], (D, SH), D ** -0.5, 0.125, ((0, 4), (1, 4)), jnp.float32)
    shared_up = bell_draw(arg_keys[8], (D, SH), D ** -0.5, 0.125, ((0, 4), (1, 4)), jnp.float32)
    shared_down = bell_draw(arg_keys[9], (SH, D), SH ** -0.5, 0.375, ((0, 4), (1, 4)), jnp.float32)
    return {"tokens": tokens, "route_ids": route_ids, "route_scores": route_scores, "norm_gain": norm_gain, "expert_gate": expert_gate, "expert_up": expert_up, "expert_down": expert_down, "shared_gate": shared_gate, "shared_up": shared_up, "shared_down": shared_down}


EPSILON = 1e-06
route_scale = 2.5

def reference(tokens, route_ids, route_scores, norm_gain, expert_gate, expert_up, expert_down, shared_gate, shared_up, shared_down):
    gain_col = norm_gain[:, None]
    sampler_gate = (gain_col[None] * expert_gate).astype(jnp.bfloat16)
    sampler_up = (gain_col[None] * expert_up).astype(jnp.bfloat16)
    sampler_down = expert_down.astype(jnp.bfloat16)
    sampler_shared_gate = (gain_col * shared_gate).astype(jnp.bfloat16)
    sampler_shared_up = (gain_col * shared_up).astype(jnp.bfloat16)
    sampler_shared_down = shared_down.astype(jnp.bfloat16)
    widened = tokens.astype(jnp.float32)
    normed = (widened * lax.rsqrt(lax.optimization_barrier(jnp.mean(widened * widened, axis=1, keepdims=True)) + EPSILON)).astype(jnp.bfloat16)
    weights = route_scale * route_scores / lax.optimization_barrier(jnp.sum(route_scores, axis=1, keepdims=True))
    gate_part = jnp.dot(normed, sampler_shared_gate, preferred_element_type=jnp.float32)
    up_part = jnp.dot(normed, sampler_shared_up, preferred_element_type=jnp.float32)
    shared_hidden = (jax.nn.silu(gate_part) * up_part).astype(jnp.bfloat16)
    shared_term = jnp.dot(shared_hidden, sampler_shared_down, preferred_element_type=jnp.float32)
    flat_ids = route_ids.reshape(-1)
    flat_weights = weights.reshape(-1)
    slots = EXPERTS * CAP

    def one_expert(expert, totals):
        matches = flat_ids == expert
        picked = jnp.nonzero(matches, size=slots, fill_value=0)[0].astype(jnp.int32)
        filled = (jnp.arange(slots, dtype=jnp.int32) < jnp.sum(matches.astype(jnp.int32))).astype(jnp.float32)
        owners = (picked // TOP_K).astype(jnp.int32)
        row_block = normed[owners]
        w_gate = lax.dynamic_index_in_dim(sampler_gate, expert, 0, keepdims=False)
        w_up = lax.dynamic_index_in_dim(sampler_up, expert, 0, keepdims=False)
        w_down = lax.dynamic_index_in_dim(sampler_down, expert, 0, keepdims=False)
        gate_rows = jnp.dot(row_block, w_gate, preferred_element_type=jnp.float32)
        up_rows = jnp.dot(row_block, w_up, preferred_element_type=jnp.float32)
        hidden = (jax.nn.silu(gate_rows) * up_rows).astype(jnp.bfloat16)
        produced = jnp.dot(hidden, w_down, preferred_element_type=jnp.float32).astype(jnp.bfloat16)
        factor = flat_weights[picked] * filled
        return totals.at[owners].add(produced.astype(jnp.float32) * factor[:, None])
    routed = lax.fori_loop(0, EXPERTS, one_expert, jnp.zeros(tokens.shape, jnp.float32))
    mixed = (routed + shared_term).astype(jnp.bfloat16)
    return (mixed, sampler_gate, sampler_up, sampler_down, sampler_shared_gate, sampler_shared_up, sampler_shared_down)
```

```python
import jax
import jax.numpy as jnp
from jax import lax
from jax.sharding import PartitionSpec as P

EPSILON = 1e-06
route_scale = 2.5


def expert_rows(row_block, w_gate, w_up, w_down):
    gate_rows = jnp.dot(row_block, w_gate, preferred_element_type=jnp.float32)
    up_rows = jnp.dot(row_block, w_up, preferred_element_type=jnp.float32)
    hidden = (jax.nn.silu(gate_rows) * up_rows).astype(jnp.bfloat16)
    return jnp.dot(hidden, w_down, preferred_element_type=jnp.float32).astype(jnp.bfloat16)


def relayout(arrived, fs_count, tp_count):
    tile_rows = arrived.shape[2]
    tile_cols = arrived.shape[3]
    grid = arrived.reshape(fs_count, tp_count, tile_rows, tile_cols)
    grid = jnp.transpose(grid, (0, 2, 1, 3))
    return grid.reshape(1, fs_count * tile_rows, tp_count * tile_cols)


def dispatch_plan(
    tokens,
    route_ids,
    route_scores,
    norm_gain,
    expert_gate,
    expert_up,
    expert_down,
    shared_gate,
    shared_up,
    shared_down,
):
    fs_count = lax.axis_size("fs")
    tp_count = lax.axis_size("tp")
    experts = fs_count * tp_count
    gain_col = norm_gain[:, None]
    piece_gate = (gain_col[None] * expert_gate).astype(jnp.bfloat16)
    piece_up = (gain_col[None] * expert_up).astype(jnp.bfloat16)
    piece_down = expert_down.astype(jnp.bfloat16)
    moved = (
        lax.all_to_all(piece_gate[:, None], ("fs", "tp"), split_axis=0, concat_axis=1, tiled=True),
        lax.all_to_all(piece_up[:, None], ("fs", "tp"), split_axis=0, concat_axis=1, tiled=True),
        lax.all_to_all(piece_down[:, None], ("fs", "tp"), split_axis=0, concat_axis=1, tiled=True),
    )
    served_gate = relayout(moved[0], fs_count, tp_count)
    served_up = relayout(moved[1], fs_count, tp_count)
    served_down = relayout(moved[2], fs_count, tp_count)
    tile_gate = (gain_col * shared_gate).astype(jnp.bfloat16)
    tile_up = (gain_col * shared_up).astype(jnp.bfloat16)
    tile_down = shared_down.astype(jnp.bfloat16)
    held_gate, held_up, held_down = (
        lax.all_gather(tile_gate, "tp", axis=1, tiled=True),
        lax.all_gather(tile_up, "tp", axis=1, tiled=True),
        lax.all_gather(tile_down, "tp", axis=1, tiled=True),
    )
    rows_dev = tokens.shape[0]
    width = tokens.shape[1]
    picks = route_ids.shape[1]
    capacity = 3 * rows_dev * picks // (2 * experts)
    widened = tokens.astype(jnp.float32)
    normed = (
        widened * lax.rsqrt(jnp.mean(widened * widened, axis=1, keepdims=True) + EPSILON)
    ).astype(jnp.bfloat16)
    weights = route_scale * route_scores / jnp.sum(route_scores, axis=1, keepdims=True)
    flat_ids = route_ids.reshape(-1)
    onehot = (flat_ids[:, None] == jnp.arange(experts, dtype=jnp.int32)[None, :]).astype(jnp.int32)
    earlier = jnp.cumsum(onehot, axis=0) - onehot
    ranks = jnp.sum(earlier * onehot, axis=1)
    target = flat_ids * capacity + ranks
    outbox = (
        jnp.zeros((experts * capacity, width), jnp.bfloat16)
        .at[target]
        .set(jnp.repeat(normed, picks, axis=0))
    )
    arrived = lax.all_to_all(
        outbox.reshape(experts, capacity, width),
        ("fs", "tp"),
        split_axis=0,
        concat_axis=0,
        tiled=True,
    )
    finished = expert_rows(
        arrived.reshape(-1, width), served_gate[0], served_up[0], served_down[0]
    ).reshape(arrived.shape)
    returned = lax.all_to_all(finished, ("fs", "tp"), split_axis=0, concat_axis=0, tiled=True)
    results = returned.reshape(experts * capacity, width)[target]
    routed = jnp.sum(
        results.reshape(rows_dev, picks, width).astype(jnp.float32) * weights[:, :, None], axis=1
    )
    columns = normed
    gate_part = jnp.dot(
        columns,
        lax.all_gather(held_gate, "fs", axis=0, tiled=True),
        preferred_element_type=jnp.float32,
    )
    up_part = jnp.dot(
        columns,
        lax.all_gather(held_up, "fs", axis=0, tiled=True),
        preferred_element_type=jnp.float32,
    )
    shared_hidden = (jax.nn.silu(gate_part) * up_part).astype(jnp.bfloat16)
    columns = shared_hidden
    shared_term = jnp.dot(
        columns,
        lax.all_gather(held_down, "fs", axis=0, tiled=True),
        preferred_element_type=jnp.float32,
    )
    mixed = (routed + shared_term).astype(jnp.bfloat16)
    return (mixed, served_gate, served_up, served_down, held_gate, held_up, held_down)


def dense_plan(
    tokens,
    route_ids,
    route_scores,
    norm_gain,
    expert_gate,
    expert_up,
    expert_down,
    shared_gate,
    shared_up,
    shared_down,
):
    fs_count = lax.axis_size("fs")
    tp_count = lax.axis_size("tp")
    experts = fs_count * tp_count
    both = ("fs", "tp")
    rows_dev, width = tokens.shape
    widened = tokens.astype(jnp.float32)
    normed = (
        widened * lax.rsqrt(jnp.mean(widened * widened, axis=1, keepdims=True) + EPSILON)
    ).astype(jnp.bfloat16)
    weights = route_scale * route_scores / jnp.sum(route_scores, axis=1, keepdims=True)
    named = route_ids[:, :, None] == jnp.arange(experts, dtype=jnp.int32)[None, None, :]
    shares = jnp.sum(jnp.where(named, weights[:, :, None], 0.0), axis=1)
    all_normed = lax.all_gather(normed, both, axis=0, tiled=True)
    own_share = lax.all_to_all(
        shares.T.reshape(experts, 1, rows_dev), both, split_axis=0, concat_axis=1, tiled=True
    ).reshape(-1)

    gain_col = norm_gain[:, None]
    piece_gate = (gain_col[None] * expert_gate).astype(jnp.bfloat16)
    piece_up = (gain_col[None] * expert_up).astype(jnp.bfloat16)
    piece_pair = jnp.concatenate([piece_gate, piece_up], axis=2)
    piece_down = expert_down.astype(jnp.bfloat16)
    pair = lax.all_to_all(piece_pair[:, None], both, split_axis=0, concat_axis=1, tiled=True)
    down = lax.all_to_all(piece_down[:, None], both, split_axis=0, concat_axis=1, tiled=True)
    cols = expert_gate.shape[2]
    served_gate = relayout(pair[:, :, :, :cols], fs_count, tp_count)
    served_up = relayout(pair[:, :, :, cols:], fs_count, tp_count)
    served_down = relayout(down, fs_count, tp_count)
    tile_gate = (gain_col * shared_gate).astype(jnp.bfloat16)
    tile_up = (gain_col * shared_up).astype(jnp.bfloat16)
    tile_down = shared_down.astype(jnp.bfloat16)
    held_gate, held_up, held_down = (
        lax.all_gather(tile_gate, "tp", axis=1, tiled=True),
        lax.all_gather(tile_up, "tp", axis=1, tiled=True),
        lax.all_gather(tile_down, "tp", axis=1, tiled=True),
    )
    gate_rows = jnp.dot(all_normed, served_gate[0], preferred_element_type=jnp.float32)
    up_rows = jnp.dot(all_normed, served_up[0], preferred_element_type=jnp.float32)
    hidden = (jax.nn.silu(gate_rows) * up_rows).astype(jnp.bfloat16)
    produced = jnp.dot(hidden, served_down[0], preferred_element_type=jnp.float32)
    partial = (produced * own_share[:, None]).astype(jnp.bfloat16)
    routed = lax.psum_scatter(partial, both, scatter_dimension=0, tiled=True)

    gate_part = jnp.dot(
        normed,
        lax.all_gather(held_gate, "fs", axis=0, tiled=True),
        preferred_element_type=jnp.float32,
    )
    up_part = jnp.dot(
        normed,
        lax.all_gather(held_up, "fs", axis=0, tiled=True),
        preferred_element_type=jnp.float32,
    )
    shared_hidden = (jax.nn.silu(gate_part) * up_part).astype(jnp.bfloat16)
    shared_term = jnp.dot(
        shared_hidden,
        lax.all_gather(held_down, "fs", axis=0, tiled=True),
        preferred_element_type=jnp.float32,
    )
    mixed = (routed.astype(jnp.float32) + shared_term).astype(jnp.bfloat16)
    return (mixed, served_gate, served_up, served_down, held_gate, held_up, held_down)


def on_device(*args):
    experts = lax.axis_size("fs") * lax.axis_size("tp")
    picks = args[1].shape[1]
    if experts <= 4 * picks:
        return dense_plan(*args)
    return dispatch_plan(*args)


def solution(mesh):
    return jax.shard_map(
        on_device,
        mesh=mesh,
        in_specs=(
            P(("grp", "fs", "tp"), None),
            P(("grp", "fs", "tp"), None),
            P(("grp", "fs", "tp"), None),
            P("fs"),
            P(None, "fs", "tp"),
            P(None, "fs", "tp"),
            P(None, "fs", "tp"),
            P("fs", "tp"),
            P("fs", "tp"),
            P("fs", "tp"),
        ),
        out_specs=(
            P(("grp", "fs", "tp"), None),
            P(("grp", "fs", "tp"), None, None),
            P(("grp", "fs", "tp"), None, None),
            P(("grp", "fs", "tp"), None, None),
            P(("grp", "fs"), None),
            P(("grp", "fs"), None),
            P(("grp", "fs"), None),
        ),
        check_vma=False,
    )
```
